256 devices in a mesh: grp: 2 (over y), ep: 32 (over z, core), tp: 4 (over x).
Axes of the slice: x: 4, y: 2, z: 16, core: 2. Of those that a mesh axis runs over, the one named last changes fastest.
The devices are a block of a 4x16x16 slice.
Arguments:
- queries: bfloat16 [24576, 1024], P(('grp', 'ep'), 'tp'), parts along dimension 0, may hold values from -6 to 6
- key_values: bfloat16 [24576, 512], P(('grp', 'ep'), 'tp'), parts along dimension 0, may hold values from -6 to 6
- query_gain: float32 [64], replicated, may hold values from 0.5 to 5
- key_gain: float32 [64], replicated, may hold values from 0.5 to 5
- out_weight: bfloat16 [1024, 2048], P('tp'), may hold values from -0.1875 to 0.1875
- second_batch: bfloat16 [32768, 2048], P(('grp', 'ep', 'tp')), parts along dimension 0, may hold values from -6 to 6
- norm_gain: float32 [2048], replicated, may hold values from 0.1 to 1.9
- routes: int32 [32768, 2], P(('grp', 'ep', 'tp')), parts along dimension 0, may hold values from 0 to 63, all different within a row; in each aligned block of 128 rows (0 to 127, 128 to 255, ...) at most 6 rows name the same one
- route_weights: float32 [32768, 2], P(('grp', 'ep', 'tp')), parts along dimension 0, may hold values from 0.2 to 1
- expert_gate: bfloat16 [64, 2048, 1024], P('ep', None, 'tp'), may hold values from -0.125 to 0.125
- expert_up: bfloat16 [64, 2048, 1024], P('ep', None, 'tp'), may hold values from -0.125 to 0.125
- expert_down: bfloat16 [64, 1024, 2048], P('ep', 'tp'), may hold values from -0.1875 to 0.1875
- shared_gate: bfloat16 [2048, 512], P(None, 'tp'), may hold values from -0.125 to 0.125
- shared_up: bfloat16 [2048, 512], P(None, 'tp'), may hold values from -0.125 to 0.125
- shared_down: bfloat16 [512, 2048], P('tp'), may hold values from -0.25 to 0.25
Outputs:
- mixer_out: bfloat16 [24576, 2048], P(('grp', 'ep', 'tp')), parts along dimension 0
- channel_out: bfloat16 [32768, 2048], P(('grp', 'ep', 'tp')), parts along dimension 0
The draws below stay inside these ranges and needn't reach their ends.
There are 2 independent parts, one for each index of `grp`. The reference program is written for one: setup_inputs(seed, part) draws one part's arguments, and reference() takes and returns one part's arrays. A program takes and returns all parts, laid end to end along the dimension named above; an argument that names none is the same for every part. Nothing has to cross between parts.
Inputs may be any that keep to these rules, and one draw needn't show every extreme that they name: `routes`: each row names 2 different experts. Among the rows of one device no expert is named more than 6 times, and in every draw some expert is named exactly 6 times by the rows of some device.
All inputs are finite; a program needn't handle non-finite values.
Results may differ from the reference program's by a relative error of at most 0.015.
The reference program's roundings to bfloat16 on the way count: a program that leaves them out, or rounds other values in their place, can miss the bound.
Values may be sent and summed in bfloat16 or wider, within the bound.
A program may use at most 128 MiB of HBM per device.

```python
import math
import jax
import jax.numpy as jnp
import numpy as np
from jax import lax

D = 2048
HEAD = 64
HQ_DEV = 4
HQ = 16
KV_HEADS = 4
GRID_W = 64
TOK_A = 384
TOKENS_A = 12288
TOK_B = 128
TOKENS_B = 16384
TOP_K = 2
EXPERTS = 64
FE_DEV = 256
EXPERT_HIDDEN = 1024
SH_DEV = 128
SHARED = 512
CAP = 6
N_EP = 32


def draw_base(key):
    keyvals = jnp.clip(jax.random.normal(jax.random.fold_in(key, 71), (TOKENS_A, KV_HEADS, 2 * HEAD), jnp.float32), -6.0, 6.0)
    queries = jnp.clip(jax.random.normal(jax.random.fold_in(key, 72), (TOKENS_A, HQ, HEAD), jnp.float32), -6.0, 6.0)
    return (queries.reshape(TOKENS_A, HQ * HEAD), keyvals.reshape(TOKENS_A, KV_HEADS * 2 * HEAD))


def draw_queries(key, part):
    return draw_base(key)[0].astype(jnp.bfloat16)


def draw_key_values(key, part):
    return draw_base(key)[1].astype(jnp.bfloat16)


def draw_gain_common(key, salt):
    return 1.0 + 0.18 * jnp.clip(jax.random.normal(jax.random.fold_in(key, salt + 1), (HEAD,), jnp.float32), -2.5, 2.5)


def draw_query_gain(key, part):
    return draw_gain_common(key, 81)


def draw_key_gain(key, part):
    return draw_gain_common(key, 91)


def block_scale(own_key, dims, pieces, low, top_value):
    def one(axis_at, shards_of):
        heights = jax.random.uniform(jax.random.fold_in(jax.random.fold_in(own_key, 6), axis_at), (shards_of,), jnp.float32, low / len(pieces), top_value / len(pieces))
        return jnp.repeat(jnp.exp(heights), dims[axis_at] // shards_of).reshape((-1,) + (1,) * (len(dims) - axis_at - 1))

    level = one(*pieces[0])
    for cut in pieces[1:]:
        level = level * one(*cut)
    return level


def assign_block(rng, own, number, rows, amount, top, reach, slope):
    ranking = jax.random.permutation(rng, amount)
    packed, ordinary = shares(amount, rows * top, reach, slope, True), shares(amount, rows * top, reach, slope, False)
    places = jnp.arange(amount)

    def named(lengths, rotation):
        used = int((lengths > 0).sum())
        fixed = max(1, used // 4)
        passed = fixed + (places - fixed + rotation * (used - fixed)) % max(1, amount - fixed)
        return jnp.zeros((amount,), jnp.int32).at[ranking[jnp.where(places < fixed, places, passed)]].set(jnp.asarray(lengths, jnp.int32))

    lengths = jnp.where(number % 4 == 0, named(packed, number // 4), named(ordinary, number - number // 4 - 1))
    mixed = jax.random.permutation(jax.random.fold_in(own, 3), amount)
    source_of, sink = mixed[0:amount // 2 * 2:2], mixed[1:amount // 2 * 2:2]
    room = jnp.minimum(lengths[source_of] - 1, reach - lengths[sink]) // 2
    room = jnp.where((source_of == ranking[0]) | (sink == ranking[0]) | (lengths[sink] == 0), 0, jnp.maximum(room, 0))
    passed = jax.random.randint(jax.random.fold_in(own, 4), (amount // 2,), 0, 1 << 20) % (room + 1)
    lengths = lengths.at[source_of].add(-passed).at[sink].add(passed)
    items = jnp.searchsorted(jnp.cumsum(lengths), jnp.arange(rows * top), side="right").astype(jnp.int32)
    grid = items.reshape(top, rows).T
    grid = grid[jax.random.permutation(jax.random.fold_in(own, 1), rows)]
    rotation = jax.random.randint(jax.random.fold_in(own, 2), (rows, 1), 0, top)
    return jnp.take_along_axis(grid, (jnp.arange(top)[None, :] + rotation) % top, axis=1)


def shares(amount, total, bound, skew, full):
    loads = [(1 << 20) // math.isqrt(rank ** skew) + 1 for rank in range(1, amount + 1)]
    largest = bound if full else min(bound, max(-(-total // amount), total * loads[0] // sum(loads)))
    least = 1 if total - largest >= amount - 1 else 0
    holding, surplus = [largest] + [least] * (amount - 1), total - largest - least * (amount - 1)
    while surplus > 0:
        candidates = [i for i in range(1, amount) if holding[i] < largest] or [i for i in range(1, amount) if holding[i] < bound]
        mass, budget = sum([loads[i] for i in candidates]), surplus
        for i in candidates:
            extra = min(bound - holding[i], max(1, budget * loads[i] // mass), surplus)
            holding[i] = holding[i] + extra
            surplus = surplus - extra
    return np.array(holding)


def centred(key, extent, width, bound, split=(), held_as=jnp.bfloat16):
    factor_of = block_scale(key, extent, split, -0.22, 0.18) if split else 1.0
    entries = jax.random.normal(key, extent, jnp.float32) * width * factor_of
    return jnp.minimum(jnp.maximum(entries, -bound), bound).astype(held_as)


def setup_inputs(seed: int = 0, part: int = 0) -> dict:
    arg_keys = jax.random.split(jax.random.key(seed), 16)
    own_keys = jax.random.split(jax.random.fold_in(arg_keys[15], part), 16)
    queries = draw_queries(jax.random.fold_in(jax.random.fold_in(arg_keys[15], part), 71), part)
    key_values = draw_key_values(jax.random.fold_in(jax.random.fold_in(arg_keys[15], part), 71), part)
    query_gain = draw_query_gain(jax.random.fold_in(arg_keys[15], 71), part)
    key_gain = draw_key_gain(jax.random.fold_in(arg_keys[15], 71), part)
    out_weight = centred(arg_keys[4], (HQ * HEAD, D), (HQ * HEAD) ** -0.5, 0.1875, ((0, 4),))
    second_batch = centred(own_keys[5], (TOKENS_B, D), 1.0, 6.0, ((0, 128),))
    norm_gain = jnp.clip(1.0 + 0.18 * jax.random.normal(arg_keys[6], (D,), jnp.float32), 0.1, 1.9)
    routes_keys = jax.random.split(jax.random.fold_in(own_keys[7], 1), TOKENS_B // TOK_B)
    routes_turns = jax.random.permutation(jax.random.fold_in(own_keys[7], 3), TOKENS_B // TOK_B)
    routes = jax.vmap(lambda own, number: assign_block(jax.random.fold_in(own_keys[7], 2), own, number, TOK_B, EXPERTS, TOP_K, CAP, 2))(routes_keys, routes_turns).reshape((TOKENS_B, TOP_K))
    route_weights = jnp.clip(0.2 + 0.8 * jax.random.uniform(own_keys[8], (TOKENS_B, TOP_K), jnp.float32) ** block_scale(own_keys[8], (TOKENS_B, TOP_K), ((0, 128),), -0.2, 0.2), 0.2, 1.0)
    expert_gate = centred(arg_keys[9], (EXPERTS, D, EXPERT_HIDDEN), D ** -0.5, 0.125, ((0, 32), (2, 4)))
    expert_up = centred(arg_keys[10], (EXPERTS, D, EXPERT_HIDDEN), D ** -0.5, 0.125, ((0, 32), (2, 4)))
    expert_down = centred(arg_keys[11], (EXPERTS, EXPERT_HIDDEN, D), EXPERT_HIDDEN ** -0.5, 0.1875, ((0, 32), (1, 4)))
    shared_gate = centred(arg_keys[12], (D, SHARED), D ** -0.5, 0.125, ((1, 4),))
    shared_up = centred(arg_keys[13], (D, SHARED), D ** -0.5, 0.125, ((1, 4),))
    shared_down = centred(arg_keys[14], (SHARED, D), SHARED ** -0.5, 0.25, ((0, 4),))
    return dict(queries=queries, key_values=key_values, query_gain=query_gain, key_gain=key_gain, out_weight=out_weight, second_batch=second_batch, norm_gain=norm_gain, routes=routes, route_weights=route_weights, expert_gate=expert_gate, expert_up=expert_up, expert_down=expert_down, shared_gate=shared_gate, shared_up=shared_up, shared_down=shared_down)


rope_base = 10000.0
norm_eps = 1e-06

def head_norm(vectors, gain):
    return vectors * lax.rsqrt(lax.optimization_barrier(jnp.mean(vectors * vectors, axis=-1, keepdims=True)) + norm_eps) * gain

def turn_heads(vectors, positions):
    row_count, head_count, head_size = vectors.shape
    half_size = head_size // 2
    inverse = rope_base ** (-jnp.arange(0, half_size, 2, dtype=jnp.float32) / half_size)
    grid_row = (positions // GRID_W).astype(jnp.float32)
    grid_column = (positions % GRID_W).astype(jnp.float32)
    angles = jnp.concatenate([grid_row[:, None] * inverse, grid_column[:, None] * inverse], axis=-1)
    cosine = jnp.cos(angles)[:, None, :]
    sine = jnp.sin(angles)[:, None, :]
    paired = vectors.reshape(row_count, head_count, half_size, 2)
    first = paired[..., 0]
    second = paired[..., 1]
    turned = jnp.stack([first * cosine - second * sine, first * sine + second * cosine], axis=-1)
    return turned.reshape(vectors.shape)

def slot_ids(route_rows, expert_count, capacity):
    row_count, top_count = route_rows.shape
    flat_routes = route_rows.reshape(-1)
    onehot = (flat_routes[:, None] == jnp.arange(expert_count, dtype=jnp.int32)[None, :]).astype(jnp.int32)
    earlier = (jnp.cumsum(onehot, axis=0).astype(jnp.int32) - onehot).astype(jnp.int32)
    within = lax.optimization_barrier(jnp.sum(earlier * onehot, axis=1)).astype(jnp.int32)
    return (flat_routes * capacity + within).astype(jnp.int32).reshape(row_count, top_count)

def slot_table(slots, slot_count):
    row_count, top_count = slots.shape
    flat_slots = slots.reshape(-1)
    owner_row = jnp.arange(row_count * top_count, dtype=jnp.int32) // top_count
    matches = flat_slots[None, :] == jnp.arange(slot_count, dtype=jnp.int32)[:, None]
    occupied = jnp.any(matches, axis=1)
    source_row = lax.optimization_barrier(jnp.sum(jnp.where(matches, owner_row[None, :], 0), axis=1)).astype(jnp.int32)
    return jnp.where(occupied, source_row, row_count).astype(jnp.int32)

def block_sum(hidden, down_weights, block_width):
    summed = jnp.zeros((hidden.shape[0], down_weights.shape[1]), jnp.float32)
    for block_index in range(hidden.shape[1] // block_width):
        lower = block_index * block_width
        partial_value = jnp.dot(hidden[:, lower:lower + block_width], down_weights[lower:lower + block_width], preferred_element_type=jnp.float32).astype(jnp.bfloat16)
        summed = summed + lax.optimization_barrier(partial_value).astype(jnp.float32)
    return summed

def swiglu_hidden(token_rows, gate_weights, up_weights):
    gate_part = jnp.dot(token_rows, gate_weights, preferred_element_type=jnp.float32)
    up_part = jnp.dot(token_rows, up_weights, preferred_element_type=jnp.float32)
    return (jax.nn.silu(gate_part) * up_part).astype(jnp.bfloat16)

def expert_apply(operands):
    slot_rows, gate_weights, up_weights, down_weights = operands
    hidden = swiglu_hidden(slot_rows, gate_weights, up_weights)
    return block_sum(hidden, down_weights, FE_DEV).astype(jnp.bfloat16)

def reference(queries, key_values, query_gain, key_gain, out_weight, second_batch, norm_gain, routes, route_weights, expert_gate, expert_up, expert_down, shared_gate, shared_up, shared_down):
    total_rows = queries.shape[0]
    positions = jnp.arange(total_rows, dtype=jnp.int32)
    query_turned = turn_heads(head_norm(queries.reshape(total_rows, HQ, HEAD).astype(jnp.float32), query_gain), positions).astype(jnp.bfloat16)
    query_turned = lax.optimization_barrier(query_turned)
    pairs = key_values.reshape(total_rows, KV_HEADS, 2 * HEAD)
    key_turned = turn_heads(head_norm(pairs[:, :, :HEAD].astype(jnp.float32), key_gain), positions).astype(jnp.bfloat16)
    key_float = lax.optimization_barrier(key_turned).astype(jnp.float32)
    value_float = pairs[:, :, HEAD:].astype(jnp.float32)
    scale = HEAD ** (-0.5)

    def query_block(block_queries):
        summed = jnp.zeros((block_queries.shape[0], D), jnp.float32)
        for head_group in range(KV_HEADS):
            group_queries = block_queries[:, head_group * HQ_DEV:(head_group + 1) * HQ_DEV].astype(jnp.float32)
            scores = jnp.einsum('qhd,kd->hqk', group_queries, key_float[:, head_group]) * scale
            top = lax.optimization_barrier(jnp.max(scores, axis=-1, keepdims=True))
            exps = jnp.exp(scores - top)
            totals = lax.optimization_barrier(jnp.sum(exps, axis=-1))
            weights = lax.optimization_barrier(exps.astype(jnp.bfloat16)).astype(jnp.float32)
            numerators = jnp.einsum('hqk,kd->qhd', weights, value_float[:, head_group])
            head_out = (numerators / totals.T[:, :, None]).astype(jnp.bfloat16).reshape(-1, HQ_DEV * HEAD)
            lower = head_group * HQ_DEV * HEAD
            partial_value = jnp.dot(head_out, out_weight[lower:lower + HQ_DEV * HEAD], preferred_element_type=jnp.float32).astype(jnp.bfloat16)
            summed = summed + lax.optimization_barrier(partial_value).astype(jnp.float32)
        return summed.astype(jnp.bfloat16)
    mixer_out = lax.map(query_block, query_turned.reshape(N_EP, TOK_A, HQ, HEAD)).reshape(total_rows, D)
    token_float = second_batch.astype(jnp.float32)
    normed = (token_float * lax.rsqrt(lax.optimization_barrier(jnp.mean(token_float * token_float, axis=-1, keepdims=True)) + norm_eps) * norm_gain).astype(jnp.bfloat16)
    block_count = normed.shape[0] // TOK_B
    slot_count = EXPERTS * CAP
    slots = jax.vmap(lambda route_rows: slot_ids(route_rows, EXPERTS, CAP))(routes.reshape(block_count, TOK_B, TOP_K))
    tables = jax.vmap(lambda slot_block: slot_table(slot_block, slot_count))(slots)
    inputs = jax.vmap(lambda token_rows, table_rows: jnp.take(token_rows, table_rows, axis=0, mode='fill', fill_value=0))(normed.reshape(block_count, TOK_B, D), tables)
    per_expert = inputs.reshape(block_count, EXPERTS, CAP, D).transpose(1, 0, 2, 3).reshape(EXPERTS, block_count * CAP, D)
    outputs = lax.map(expert_apply, (per_expert, expert_gate, expert_up, expert_down))
    by_block = outputs.reshape(EXPERTS, block_count, CAP, D).transpose(1, 0, 2, 3).reshape(block_count, slot_count, D)
    chosen = jax.vmap(lambda block_out, slot_block: jnp.take(block_out, slot_block.reshape(-1), axis=0))(by_block, slots).reshape(-1, TOP_K, D)
    routed = lax.optimization_barrier(jnp.sum(route_weights[:, :, None] * chosen.astype(jnp.float32), axis=1))
    shared_hidden = swiglu_hidden(normed, shared_gate, shared_up)
    shared_sum = block_sum(shared_hidden, shared_down, SH_DEV)
    channel_out = (shared_sum + routed).astype(jnp.bfloat16)
    return (mixer_out, channel_out)
```

```python
import functools

import jax
import jax.numpy as jnp
from jax import lax
from jax.experimental import pallas as pl
from jax.experimental.pallas import tpu as pltpu
from jax.sharding import Mesh
from jax.sharding import PartitionSpec as P

GRID_W = 64
EP = ("ep_0", "ep_1")
GRP_EP = ("grp", "ep_0", "ep_1")
GRP_EP_TP = ("grp", "ep_0", "ep_1", "tp")
MESH = pl.DeviceIdType.MESH
BF = jnp.bfloat16
F32 = jnp.float32
rope_base = 10000.0
norm_eps = 1e-06
LOG2E = 1.4426950408889634
VMEM_BYTES = 60 * 1024 * 1024
CAPACITY = 6
SPLIT = 4


def vspec():
    return pl.BlockSpec(memory_space=pltpu.VMEM)


def local_call(kernel, outs, flops, name, scratch=(), vmem=VMEM_BYTES):
    def call(*args):
        size = sum(a.size * a.dtype.itemsize for a in (*args, *outs))
        return pl.pallas_call(
            kernel,
            in_specs=[vspec()] * len(args),
            out_specs=[vspec()] * len(outs),
            out_shape=list(outs),
            scratch_shapes=list(scratch),
            compiler_params=pltpu.CompilerParams(vmem_limit_bytes=vmem),
            cost_estimate=pl.CostEstimate(flops=flops, bytes_accessed=size, transcendentals=0),
            name=name,
        )(*args)

    return call


def iota(shape, dim):
    return lax.broadcasted_iota(jnp.int32, shape, dim)


def mm(a, b):
    return jnp.dot(a, b, preferred_element_type=F32)


def slots_in_lanes(routes_t, experts):
    tokens = routes_t.shape[1]
    row = iota((experts, tokens), 0)
    first = (row == routes_t[0:1, :]).astype(F32)
    second = (row == routes_t[1:2, :]).astype(F32)
    before = (iota((tokens, tokens), 0) < iota((tokens, tokens), 1)).astype(BF)
    counts = mm((first + second).astype(BF), before)
    out = []
    for k, hot in enumerate((first, second)):
        within = jnp.sum(counts * hot, axis=0, keepdims=True).astype(jnp.int32)
        out.append(routes_t[k : k + 1, :] * CAPACITY + within)
    return out


def slots_in_rows(routes, experts):
    tokens = routes.shape[0]
    col = iota((tokens, experts), 1)
    first = (col == routes[:, 0:1]).astype(F32)
    second = (col == routes[:, 1:2]).astype(F32)
    before = (iota((tokens, tokens), 1) < iota((tokens, tokens), 0)).astype(BF)
    counts = mm(before, (first + second).astype(BF))
    out = []
    for k, hot in enumerate((first, second)):
        within = jnp.sum(counts * hot, axis=1, keepdims=True).astype(jnp.int32)
        out.append(routes[:, k : k + 1] * CAPACITY + within)
    return out


def slot_of_row(row, local_experts, j):
    per = CAPACITY * SPLIT
    dest = row // per
    quarter = (row % per) // CAPACITY
    place = row % CAPACITY
    return (dest * local_experts + j) * CAPACITY + place, quarter


def prep_kernel(x_ref, gain_ref, routes_t_ref, normed_ref, *chunk_refs, experts, local_experts):
    x = x_ref[...].astype(F32)
    scale = lax.rsqrt(jnp.mean(x * x, axis=-1, keepdims=True) + norm_eps)
    normed_ref[...] = (x * scale * gain_ref[...]).astype(BF)
    tokens, width = x_ref.shape
    piece = width // SPLIT
    slots = slots_in_lanes(routes_t_ref[...], experts)
    for j, out_ref in enumerate(chunk_refs):
        rows = out_ref.shape[0]
        slot, _ = slot_of_row(iota((rows, tokens), 0), local_experts, j)
        hot = ((slot == slots[0]) | (slot == slots[1])).astype(BF)
        _, quarter = slot_of_row(iota((rows, piece), 0), local_experts, j)
        got = jnp.zeros((rows, piece), F32)
        for q in range(SPLIT):
            part = mm(hot, normed_ref[:, q * piece : (q + 1) * piece])
            got = jnp.where(quarter == q, part, got)
        out_ref[...] = got.astype(BF)


def sorter(group):
    per = CAPACITY * SPLIT
    rows = group * per
    to = iota((rows, rows), 0)
    at = iota((rows, rows), 1)
    quarter = to // (group * CAPACITY)
    source = (to % (group * CAPACITY)) // CAPACITY
    place = to % CAPACITY
    return (at == source * per + quarter * CAPACITY + place).astype(BF)


def unsorter(group):
    per = CAPACITY * SPLIT
    rows = group * per
    to = iota((rows, rows), 1)
    at = iota((rows, rows), 0)
    quarter = to // (group * CAPACITY)
    source = (to % (group * CAPACITY)) // CAPACITY
    place = to % CAPACITY
    return (at == source * per + quarter * CAPACITY + place).astype(BF)


def silu(v):
    return v / (1.0 + jnp.exp(-v))


GROUP = 8


def experts_kernel(*refs, parts):
    x_refs = refs[: sum(len(p) for p in parts)]
    gate_ref, up_ref, down_ref = refs[len(x_refs) : len(x_refs) + 3]
    o_refs = refs[len(x_refs) + 3 : len(x_refs) + 3 + len(parts)]
    a_ref, h_ref = refs[len(x_refs) + 3 + len(parts) :]
    per = CAPACITY * SPLIT
    grows = GROUP * per
    places = GROUP * CAPACITY
    piece = x_refs[0].shape[1]
    order = sorter(GROUP)
    back = unsorter(GROUP)
    at = 0
    for p, o_ref in zip(parts, o_refs):
        group = 0
        for part in p:
            x_ref = x_refs[at]
            at += 1
            for g in range(x_ref.shape[0] // grows):
                block = mm(order, x_ref[g * grows : (g + 1) * grows, :]).astype(BF)
                for q in range(SPLIT):
                    a_ref[group * places : (group + 1) * places, q * piece : (q + 1) * piece] = (
                        block[q * places : (q + 1) * places, :]
                    )
                group += 1
        rows = group * places
        gate = mm(a_ref[0:rows, :], gate_ref[0])
        up = mm(a_ref[0:rows, :], up_ref[0])
        h_ref[...] = (silu(gate) * up).astype(BF)
        for g in range(group):
            here = h_ref[g * places : (g + 1) * places, :]
            stacked = jnp.concatenate(
                [
                    mm(here, down_ref[0, :, q * piece : (q + 1) * piece]).astype(BF)
                    for q in range(SPLIT)
                ],
                axis=0,
            )
            o_ref[g * grows : (g + 1) * grows, :] = mm(back, stacked).astype(BF)


def run_experts(pieces, parts, weights, j):
    rows, piece = pieces[0].shape
    gate, up, down = weights
    width, hidden = gate.shape[1:]
    outs = [jax.ShapeDtypeStruct((rows, piece), BF)] * len(parts)
    total = rows * len(parts) // SPLIT
    return pl.pallas_call(
        functools.partial(experts_kernel, parts=parts),
        grid=(1,),
        in_specs=[pl.BlockSpec(p.shape, lambda i: (0, 0)) for p in pieces]
        + [
            pl.BlockSpec((1, width, hidden), lambda i: (j, 0, 0)),
            pl.BlockSpec((1, width, hidden), lambda i: (j, 0, 0)),
            pl.BlockSpec((1, hidden, width), lambda i: (j, 0, 0)),
        ],
        out_specs=[pl.BlockSpec((rows, piece), lambda i: (0, 0))] * len(parts),
        out_shape=outs,
        scratch_shapes=[
            pltpu.VMEM((rows // SPLIT, width), BF),
            pltpu.VMEM((rows // SPLIT, hidden), BF),
        ],
        compiler_params=pltpu.CompilerParams(vmem_limit_bytes=VMEM_BYTES),
        cost_estimate=pl.CostEstimate(
            flops=6 * total * width * hidden,
            bytes_accessed=4 * rows * piece * len(parts) + 6 * width * hidden,
            transcendentals=0,
        ),
        name=f"experts_{j}",
    )(*pieces, gate, up, down)


def shared_kernel(*refs):
    x_refs = refs[:4]
    gate_ref, up_ref, down_ref = refs[4:7]
    o_refs = refs[7:]
    for x_ref, o_ref in zip(x_refs, o_refs):
        gate = mm(x_ref[...], gate_ref[...])
        up = mm(x_ref[...], up_ref[...])
        hidden = (silu(gate) * up).astype(BF)
        o_ref[...] = mm(hidden, down_ref[...]).astype(BF)


def combine_kernel(*refs, experts, local_experts):
    shared_refs = refs[:4]
    routes_ref, weights_ref = refs[4:6]
    back_refs = refs[6:-1]
    o_ref = refs[-1]
    tokens = routes_ref.shape[0]
    slots = slots_in_rows(routes_ref[...], experts)
    piece = back_refs[0].shape[1]
    rows = back_refs[0].shape[0]
    slot_id = []
    for j in range(len(back_refs)):
        slot_id.append(slot_of_row(iota((tokens, rows), 1), local_experts, j))
    for q in range(SPLIT):
        cols = slice(q * piece, (q + 1) * piece)
        total = shared_refs[0][:, cols].astype(F32)
        for ref in shared_refs[1:]:
            total = total + ref[:, cols].astype(F32)
        for k in range(2):
            picked = jnp.zeros((tokens, piece), F32)
            for j, back_ref in enumerate(back_refs):
                slot, quarter = slot_id[j]
                hot = ((slot == slots[k]) & (quarter == q)).astype(BF)
                picked = picked + mm(hot, back_ref[...])
            total = total + weights_ref[:, k : k + 1] * picked
        o_ref[:, cols] = total.astype(BF)


def turn_kernel(q_ref, kv_ref, qgain_ref, kgain_ref, cos_ref, sin_ref, q_out_ref, kv_out_ref):
    head = qgain_ref.shape[1]
    heads = q_ref.shape[1] // head
    rows = q_ref.shape[0]
    even = iota((rows, 2 * head), 1) % 2 == 0

    def normed(v, gain):
        return v * lax.rsqrt(jnp.mean(v * v, axis=-1, keepdims=True) + norm_eps) * gain

    def turned(pair):
        after = pltpu.roll(pair, 2 * head - 1, 1)
        before = pltpu.roll(pair, 1, 1)
        other = jnp.where(even, after, before)
        return pair * cos_ref[...] + other * sin_ref[...]

    scale = LOG2E * head**-0.5
    for h in range(0, heads, 2):
        pair = jnp.concatenate(
            [
                normed(q_ref[:, (h + i) * head : (h + i + 1) * head].astype(F32), qgain_ref[...])
                for i in range(2)
            ],
            axis=1,
        )
        both = turned(pair).astype(BF).astype(F32) * scale
        for i in range(2):
            one = both[:, i * head : (i + 1) * head]
            high = one.astype(BF)
            low = (one - high.astype(F32)).astype(BF)
            q_out_ref[(h + i) * rows : (h + i + 1) * rows, :] = jnp.concatenate([high, low], axis=1)
    key = normed(kv_ref[:, :head].astype(F32), kgain_ref[...])
    key = turned(jnp.concatenate([key, key], axis=1)).astype(BF)
    kv_out_ref[...] = jnp.concatenate([key[:, :head], kv_ref[:, head:]], axis=1)


def angle_tables(positions, head):
    half = head // 2
    inverse = rope_base ** (-jnp.arange(0, half, 2, dtype=F32) / half)
    lane = jnp.arange(2 * head, dtype=jnp.int32) % head
    which = lane // 2
    grid_row = (positions // GRID_W).astype(F32)
    grid_column = (positions % GRID_W).astype(F32)
    both = jnp.concatenate([inverse, inverse])[which]
    place = jnp.where(which[None, :] < half // 2, grid_row[:, None], grid_column[:, None])
    angles = place * both[None, :]
    sign = jnp.where(lane % 2 == 0, -1.0, 1.0)
    return jnp.cos(angles), jnp.sin(angles) * sign[None, :]


def gather_kernel(x_ref, o_ref, ssem, rsem, dsem, drsem, lsem):
    z = lax.axis_index("ep_0")
    core = lax.axis_index("ep_1")
    count = lax.axis_size("ep_0")
    right = lax.rem(z + 1, count)
    left = lax.rem(z + count - 1, count)
    twin = 1 - core
    barrier = pltpu.get_barrier_semaphore()
    for peer in ({"ep_0": right}, {"ep_0": left}, {"ep_1": twin}):
        pl.semaphore_signal(barrier, 1, device_id=peer, device_id_type=MESH)
    pl.semaphore_wait(barrier, 3)

    def slot(at):
        return o_ref.at[lax.rem(at + 2 * count, count) * 2 + core]

    def ring(step, way, src, at):
        return pltpu.make_async_remote_copy(
            src_ref=src,
            dst_ref=slot(at),
            send_sem=ssem.at[way, step],
            recv_sem=rsem.at[way, step],
            device_id={"ep_0": left if way else right},
            device_id_type=MESH,
        )

    def across(k, src, at):
        return pltpu.make_async_remote_copy(
            src_ref=src,
            dst_ref=slot(at),
            send_sem=dsem.at[k],
            recv_sem=drsem.at[k],
            device_id={"ep_1": twin},
            device_id_type=MESH,
        )

    own = pltpu.make_async_copy(x_ref, slot(z), lsem)
    own.start()
    to_right = [ring(0, 0, x_ref, z)]
    to_left = [ring(0, 1, x_ref, z)]
    to_right[0].start()
    to_left[0].start()
    swaps = [across(0, x_ref, z)]
    swaps[0].start()
    steps_right = count // 2
    steps_left = count - 1 - steps_right
    for step in range(1, steps_right + 1):
        to_right[step - 1].wait_recv()
        if step < steps_right:
            to_right.append(ring(step, 0, slot(z - step), z - step))
            to_right[-1].start()
        swaps.append(across(len(swaps), slot(z - step), z - step))
        swaps[-1].start()
        if step <= steps_left:
            to_left[step - 1].wait_recv()
            if step < steps_left:
                to_left.append(ring(step, 1, slot(z + step), z + step))
                to_left[-1].start()
            swaps.append(across(len(swaps), slot(z + step), z + step))
            swaps[-1].start()
    for copy in to_right + to_left:
        copy.wait_send()
    for copy in swaps:
        copy.wait()
    own.wait()


def gather_keys(block):
    count = lax.axis_size("ep_0")
    half = count // 2
    return pl.pallas_call(
        gather_kernel,
        in_specs=[vspec()],
        out_specs=vspec(),
        out_shape=jax.ShapeDtypeStruct((2 * count, *block.shape), block.dtype),
        scratch_shapes=[
            pltpu.SemaphoreType.DMA((2, half)),
            pltpu.SemaphoreType.DMA((2, half)),
            pltpu.SemaphoreType.DMA((count,)),
            pltpu.SemaphoreType.DMA((count,)),
            pltpu.SemaphoreType.DMA,
        ],
        compiler_params=pltpu.CompilerParams(
            collective_id=0, has_side_effects=True, vmem_limit_bytes=16 * 1024 * 1024
        ),
        cost_estimate=pl.CostEstimate(
            flops=1 << 28, bytes_accessed=64 * block.size, transcendentals=0
        ),
        name="gather_keys",
    )(block)


def attend_kernel(q_ref, kv_ref, o_ref, *, key_block, query_tile):
    head = q_ref.shape[1] // 2
    lane = iota((key_block, 2 * head), 1)
    tiles = q_ref.shape[0] // query_tile

    def step(i, carried):
        block = kv_ref[pl.ds(pl.multiple_of(i * key_block, key_block), key_block), :]
        keys = jnp.concatenate([block[:, :head], block[:, :head]], axis=1)
        values = jnp.where(lane < head, jnp.ones_like(block), block)
        out = []
        for t in range(tiles):
            top, acc = carried[t]
            scores = lax.dot_general(
                q_ref[t * query_tile : (t + 1) * query_tile, :],
                keys,
                (((1,), (1,)), ((), ())),
                preferred_element_type=F32,
            )
            top_new = jnp.maximum(top, jnp.max(scores, axis=1, keepdims=True))
            weights = jnp.exp2(scores - top_new).astype(BF)
            out.append((top_new, acc * jnp.exp2(top - top_new) + mm(weights, values)))
        return tuple(out)

    start = tuple(
        (jnp.full((query_tile, 1), -1e30, F32), jnp.zeros((query_tile, 2 * head), F32))
        for _ in range(tiles)
    )
    ended = lax.fori_loop(0, kv_ref.shape[0] // key_block, step, start)
    for t in range(tiles):
        _, acc = ended[t]
        o_ref[t * query_tile : (t + 1) * query_tile, :] = (acc[:, head:] / acc[:, :1]).astype(BF)


def attend(q_rows, kv, query_tile):
    rows = q_rows.shape[0]
    keys, both = kv.shape
    key_block = next(b for b in (2048, 1024, 512, 256, 128, keys) if keys % b == 0)
    return local_call(
        functools.partial(attend_kernel, key_block=key_block, query_tile=query_tile),
        [jax.ShapeDtypeStruct((rows, both // 2), BF)],
        12 * rows * keys * both,
        "attend",
    )(q_rows, kv)[0]


def moved(x, by):
    count = lax.axis_size("tp")
    return lax.ppermute(x, "tp", [(i, (i + by) % count) for i in range(count)])


def summed(parts):
    total = parts[0].astype(F32)
    for part in parts[1:]:
        total = total + part.astype(F32)
    return total


def body(
    queries,
    key_values,
    query_gain,
    key_gain,
    out_weight,
    second_batch,
    norm_gain,
    routes,
    route_weights,
    expert_gate,
    expert_up,
    expert_down,
    shared_gate,
    shared_up,
    shared_down,
):
    rows = queries.shape[0]
    head = query_gain.shape[0]
    heads = queries.shape[1] // head
    ep_count = lax.axis_size(EP)
    tp_count = lax.axis_size("tp")
    tokens, width = second_batch.shape
    local_experts = expert_gate.shape[0]
    experts = local_experts * ep_count
    piece = width // SPLIT
    chunk_rows = ep_count * CAPACITY * SPLIT
    chunk = jax.ShapeDtypeStruct((chunk_rows, piece), BF)

    normed, *outgoing = local_call(
        functools.partial(prep_kernel, experts=experts, local_experts=local_experts),
        [jax.ShapeDtypeStruct((tokens, width), BF)] + [chunk] * local_experts,
        2 * local_experts * chunk_rows * tokens * width,
        "prep",
    )(second_batch, norm_gain[None, :], routes.T)

    def across(x):
        tiles = x.reshape(ep_count, -1, piece)
        return lax.all_to_all(tiles, EP, split_axis=0, concat_axis=0, tiled=True).reshape(x.shape)

    positions = lax.axis_index(EP) * rows + jnp.arange(rows, dtype=jnp.int32)
    cosine, sine = angle_tables(positions, head)
    q_rows, kv_block = local_call(
        turn_kernel,
        [
            jax.ShapeDtypeStruct((heads * rows, 2 * head), BF),
            jax.ShapeDtypeStruct((rows, 2 * head), BF),
        ],
        1 << 26,
        "turn",
    )(queries, key_values, query_gain[None, :], key_gain[None, :], cosine, sine)
    kv = gather_keys(kv_block).reshape(ep_count * rows, 2 * head)

    near = [moved(normed, 1), moved(normed, -1), moved(normed, 2)]
    partial = local_call(
        shared_kernel,
        [jax.ShapeDtypeStruct((tokens, width), BF)] * 4,
        6 * 4 * tokens * width * shared_gate.shape[1],
        "shared",
    )(normed, *near, shared_gate, shared_up, shared_down)
    shared_parts = [
        partial[0],
        moved(partial[1], -1),
        moved(partial[2], 1),
        moved(partial[3], 2),
    ]

    weights = (expert_gate, expert_up, expert_down)
    returned = []
    half = chunk_rows // 2
    for j in range(local_experts):
        mine = across(outgoing[j])
        from_left = moved(mine, 1)
        from_right = moved(mine, -1)
        far_low = moved(from_left[:half], 1)
        far_high = moved(from_right[half:], -1)
        out = run_experts(
            (mine, from_left, from_right, far_low, far_high),
            ((0,), (1,), (2,), (3, 4)),
            weights,
            j,
        )
        arrived = [out[0], moved(out[1], -1), moved(out[2], 1), moved(out[3], 2)]
        returned.append(across(summed(arrived).astype(BF)))

    attended = [attend(q_rows[h * rows : (h + 1) * rows], kv, rows) for h in range(heads)]
    head_out = jnp.concatenate(attended, axis=1)
    me = lax.axis_index("tp")
    block = rows // tp_count

    def partial_for(by):
        at = lax.rem(me + by + tp_count, tp_count) * block
        own = lax.dynamic_slice_in_dim(head_out, at, block, 0)
        return jnp.dot(own, out_weight, preferred_element_type=F32).astype(BF)

    attn_sum = summed(
        [
            partial_for(0),
            moved(partial_for(1), 1),
            moved(partial_for(-1), -1),
            moved(partial_for(2), 2),
        ]
    )

    combined = local_call(
        functools.partial(combine_kernel, experts=experts, local_experts=local_experts),
        [jax.ShapeDtypeStruct((tokens, width), BF)],
        4 * local_experts * chunk_rows * tokens * width,
        "combine",
    )(*shared_parts, routes, route_weights, *returned)[0]
    return (attn_sum.astype(BF), combined)


def solution(mesh):
    torus = Mesh(
        mesh.devices.reshape(mesh.shape["grp"], mesh.shape["ep"] // 2, 2, mesh.shape["tp"]),
        ("grp", "ep_0", "ep_1", "tp"),
    )
    return jax.shard_map(
        body,
        mesh=torus,
        in_specs=(
            P(GRP_EP, "tp"),
            P(GRP_EP, "tp"),
            P(),
            P(),
            P("tp", None),
            P(GRP_EP_TP, None),
            P(),
            P(GRP_EP_TP, None),
            P(GRP_EP_TP, None),
            P(EP, None, "tp"),
            P(EP, None, "tp"),
            P(EP, "tp", None),
            P(None, "tp"),
            P(None, "tp"),
            P("tp", None),
        ),
        out_specs=(P(GRP_EP_TP, None), P(GRP_EP_TP, None)),
        check_vma=False,
    )
```

```python
import functools

import jax
import jax.numpy as jnp
from jax import lax
from jax.experimental import pallas as pl
from jax.experimental.pallas import tpu as pltpu
from jax.sharding import Mesh
from jax.sharding import PartitionSpec as P

GRID_W = 64
EP = ("ep_0", "ep_1")
GRP_EP = ("grp", "ep_0", "ep_1")
GRP_EP_TP = ("grp", "ep_0", "ep_1", "tp")
MESH = pl.DeviceIdType.MESH
BF = jnp.bfloat16
F32 = jnp.float32
rope_base = 10000.0
norm_eps = 1e-06
LOG2E = 1.4426950408889634
VMEM_BYTES = 60 * 1024 * 1024
CAPACITY = 6
SPLIT = 4


def vspec():
    return pl.BlockSpec(memory_space=pltpu.VMEM)


def local_call(kernel, outs, flops, scratch=(), vmem=VMEM_BYTES):
    def call(*args):
        size = sum(a.size * a.dtype.itemsize for a in (*args, *outs))
        return pl.pallas_call(
            kernel,
            in_specs=[vspec()] * len(args),
            out_specs=[vspec()] * len(outs),
            out_shape=list(outs),
            scratch_shapes=list(scratch),
            compiler_params=pltpu.CompilerParams(vmem_limit_bytes=vmem),
            cost_estimate=pl.CostEstimate(flops=flops, bytes_accessed=size, transcendentals=0),
        )(*args)

    return call


def iota(shape, dim):
    return lax.broadcasted_iota(jnp.int32, shape, dim)


def mm(a, b):
    return jnp.dot(a, b, preferred_element_type=F32)


def slots_in_lanes(routes_t, experts):
    tokens = routes_t.shape[1]
    row = iota((experts, tokens), 0)
    first = (row == routes_t[0:1, :]).astype(F32)
    second = (row == routes_t[1:2, :]).astype(F32)
    before = (iota((tokens, tokens), 0) < iota((tokens, tokens), 1)).astype(BF)
    counts = mm((first + second).astype(BF), before)
    out = []
    for k, hot in enumerate((first, second)):
        within = jnp.sum(counts * hot, axis=0, keepdims=True).astype(jnp.int32)
        out.append(routes_t[k : k + 1, :] * CAPACITY + within)
    return out


def slots_in_rows(routes, experts):
    tokens = routes.shape[0]
    col = iota((tokens, experts), 1)
    first = (col == routes[:, 0:1]).astype(F32)
    second = (col == routes[:, 1:2]).astype(F32)
    before = (iota((tokens, tokens), 1) < iota((tokens, tokens), 0)).astype(BF)
    counts = mm(before, (first + second).astype(BF))
    out = []
    for k, hot in enumerate((first, second)):
        within = jnp.sum(counts * hot, axis=1, keepdims=True).astype(jnp.int32)
        out.append(routes[:, k : k + 1] * CAPACITY + within)
    return out


def slot_of_row(row, local_experts, j):
    per = CAPACITY * SPLIT
    dest = row // per
    quarter = (row % per) // CAPACITY
    place = row % CAPACITY
    return (dest * local_experts + j) * CAPACITY + place, quarter


def prep_kernel(x_ref, gain_ref, routes_t_ref, normed_ref, *chunk_refs, experts, local_experts):
    x = x_ref[...].astype(F32)
    scale = lax.rsqrt(jnp.mean(x * x, axis=-1, keepdims=True) + norm_eps)
    normed_ref[...] = (x * scale * gain_ref[...]).astype(BF)
    tokens, width = x_ref.shape
    piece = width // SPLIT
    slots = slots_in_lanes(routes_t_ref[...], experts)
    for j, out_ref in enumerate(chunk_refs):
        rows = out_ref.shape[0]
        slot, _ = slot_of_row(iota((rows, tokens), 0), local_experts, j)
        hot = ((slot == slots[0]) | (slot == slots[1])).astype(BF)
        _, quarter = slot_of_row(iota((rows, piece), 0), local_experts, j)
        got = jnp.zeros((rows, piece), F32)
        for q in range(SPLIT):
            part = mm(hot, normed_ref[:, q * piece : (q + 1) * piece])
            got = jnp.where(quarter == q, part, got)
        out_ref[...] = got.astype(BF)


def sorter(group):
    per = CAPACITY * SPLIT
    rows = group * per
    to = iota((rows, rows), 0)
    at = iota((rows, rows), 1)
    quarter = to // (group * CAPACITY)
    source = (to % (group * CAPACITY)) // CAPACITY
    place = to % CAPACITY
    return (at == source * per + quarter * CAPACITY + place).astype(BF)


def unsorter(group):
    per = CAPACITY * SPLIT
    rows = group * per
    to = iota((rows, rows), 1)
    at = iota((rows, rows), 0)
    quarter = to // (group * CAPACITY)
    source = (to % (group * CAPACITY)) // CAPACITY
    place = to % CAPACITY
    return (at == source * per + quarter * CAPACITY + place).astype(BF)


def silu(v):
    return v / (1.0 + jnp.exp(-v))


GROUP = 8


def experts_kernel(*refs, parts):
    x_refs = refs[: sum(len(p) for p in parts)]
    gate_ref, up_ref, down_ref = refs[len(x_refs) : len(x_refs) + 3]
    o_refs = refs[len(x_refs) + 3 : len(x_refs) + 3 + len(parts)]
    a_ref, h_ref = refs[len(x_refs) + 3 + len(parts) :]
    per = CAPACITY * SPLIT
    grows = GROUP * per
    places = GROUP * CAPACITY
    piece = x_refs[0].shape[1]
    order = sorter(GROUP)
    back = unsorter(GROUP)
    at = 0
    group = 0
    for p in parts:
        for part in p:
            x_ref = x_refs[at]
            at += 1
            for g in range(x_ref.shape[0] // grows):
                block = mm(order, x_ref[g * grows : (g + 1) * grows, :]).astype(BF)
                for q in range(SPLIT):
                    a_ref[group * places : (group + 1) * places, q * piece : (q + 1) * piece] = block[q * places : (q + 1) * places, :]
                group += 1
    gate = mm(a_ref[...], gate_ref[0])
    up = mm(a_ref[...], up_ref[0])
    h_ref[...] = (silu(gate) * up).astype(BF)
    for q in range(SPLIT):
        a_ref[:, q * piece : (q + 1) * piece] = mm(h_ref[...], down_ref[0, :, q * piece : (q + 1) * piece]).astype(BF)
    per_part = group // len(o_refs)
    for k, o_ref in enumerate(o_refs):
        for g in range(per_part):
            lo = (k * per_part + g) * places
            stacked = jnp.concatenate([a_ref[lo : lo + places, q * piece : (q + 1) * piece] for q in range(SPLIT)], axis=0)
            o_ref[g * grows : (g + 1) * grows, :] = mm(back, stacked).astype(BF)


def run_experts(pieces, parts, weights, j):
    rows, piece = pieces[0].shape
    gate, up, down = weights
    width, hidden = gate.shape[1:]
    outs = [jax.ShapeDtypeStruct((rows, piece), BF)] * len(parts)
    total = rows * len(parts) // SPLIT
    return pl.pallas_call(
        functools.partial(experts_kernel, parts=parts),
        grid=(1,),
        in_specs=[pl.BlockSpec(p.shape, lambda i: (0, 0)) for p in pieces]
        + [
            pl.BlockSpec((1, width, hidden), lambda i: (j, 0, 0)),
            pl.BlockSpec((1, width, hidden), lambda i: (j, 0, 0)),
            pl.BlockSpec((1, hidden, width), lambda i: (j, 0, 0)),
        ],
        out_specs=[pl.BlockSpec((rows, piece), lambda i: (0, 0))] * len(parts),
        out_shape=outs,
        scratch_shapes=[
            pltpu.VMEM((total, width), BF),
            pltpu.VMEM((total, hidden), BF),
        ],
        compiler_params=pltpu.CompilerParams(vmem_limit_bytes=VMEM_BYTES),
        cost_estimate=pl.CostEstimate(
            flops=6 * total * width * hidden,
            bytes_accessed=4 * rows * piece * len(parts) + 6 * width * hidden,
            transcendentals=0,
        ),
    )(*pieces, gate, up, down)


def shared_kernel(*refs):
    x_refs = refs[:4]
    gate_ref, up_ref, down_ref = refs[4:7]
    o_refs = refs[7:]
    for x_ref, o_ref in zip(x_refs, o_refs):
        gate = mm(x_ref[...], gate_ref[...])
        up = mm(x_ref[...], up_ref[...])
        hidden = (silu(gate) * up).astype(BF)
        o_ref[...] = mm(hidden, down_ref[...]).astype(BF)


def combine_kernel(*refs, experts, local_experts):
    shared_refs = refs[:4]
    routes_ref, weights_ref = refs[4:6]
    back_refs = refs[6:-1]
    o_ref = refs[-1]
    tokens = routes_ref.shape[0]
    slots = slots_in_rows(routes_ref[...], experts)
    piece = back_refs[0].shape[1]
    rows = back_refs[0].shape[0]
    slot_id = []
    for j in range(len(back_refs)):
        slot_id.append(slot_of_row(iota((tokens, rows), 1), local_experts, j))
    for q in range(SPLIT):
        cols = slice(q * piece, (q + 1) * piece)
        total = shared_refs[0][:, cols].astype(F32)
        for ref in shared_refs[1:]:
            total = total + ref[:, cols].astype(F32)
        for k in range(2):
            picked = jnp.zeros((tokens, piece), F32)
            for j, back_ref in enumerate(back_refs):
                slot, quarter = slot_id[j]
                hot = ((slot == slots[k]) & (quarter == q)).astype(BF)
                picked = picked + mm(hot, back_ref[...])
            total = total + weights_ref[:, k : k + 1] * picked
        o_ref[:, cols] = total.astype(BF)


def turn_kernel(q_ref, kv_ref, qgain_ref, kgain_ref, cos_ref, sin_ref, q_out_ref, kv_out_ref):
    head = qgain_ref.shape[1]
    heads = q_ref.shape[1] // head
    rows = q_ref.shape[0]
    even = iota((rows, 2 * head), 1) % 2 == 0

    def normed(v, gain):
        return v * lax.rsqrt(jnp.mean(v * v, axis=-1, keepdims=True) + norm_eps) * gain

    def turned(pair):
        after = pltpu.roll(pair, 2 * head - 1, 1)
        before = pltpu.roll(pair, 1, 1)
        other = jnp.where(even, after, before)
        return pair * cos_ref[...] + other * sin_ref[...]

    scale = LOG2E * head**-0.5
    for h in range(0, heads, 2):
        pair = jnp.concatenate(
            [
                normed(q_ref[:, (h + i) * head : (h + i + 1) * head].astype(F32), qgain_ref[...])
                for i in range(2)
            ],
            axis=1,
        )
        both = turned(pair).astype(BF).astype(F32) * scale
        for i in range(2):
            one = both[:, i * head : (i + 1) * head]
            high = one.astype(BF)
            low = (one - high.astype(F32)).astype(BF)
            q_out_ref[(h + i) * rows : (h + i + 1) * rows, :] = jnp.concatenate([high, low], axis=1)
    key = normed(kv_ref[:, :head].astype(F32), kgain_ref[...])
    key = turned(jnp.concatenate([key, key], axis=1)).astype(BF)
    kv_out_ref[...] = jnp.concatenate([key[:, :head], kv_ref[:, head:]], axis=1)


def angle_tables(positions, head):
    half = head // 2
    inverse = rope_base ** (-jnp.arange(0, half, 2, dtype=F32) / half)
    lane = jnp.arange(2 * head, dtype=jnp.int32) % head
    which = lane // 2
    grid_row = (positions // GRID_W).astype(F32)
    grid_column = (positions % GRID_W).astype(F32)
    both = jnp.concatenate([inverse, inverse])[which]
    place = jnp.where(which[None, :] < half // 2, grid_row[:, None], grid_column[:, None])
    angles = place * both[None, :]
    sign = jnp.where(lane % 2 == 0, -1.0, 1.0)
    return jnp.cos(angles), jnp.sin(angles) * sign[None, :]


def gather_kernel(x_ref, o_ref, ssem, rsem, dsem, drsem, lsem):
    z = lax.axis_index("ep_0")
    core = lax.axis_index("ep_1")
    count = lax.axis_size("ep_0")
    right = lax.rem(z + 1, count)
    left = lax.rem(z + count - 1, count)
    twin = 1 - core
    barrier = pltpu.get_barrier_semaphore()
    for peer in ({"ep_0": right}, {"ep_0": left}, {"ep_1": twin}):
        pl.semaphore_signal(barrier, 1, device_id=peer, device_id_type=MESH)
    pl.semaphore_wait(barrier, 3)

    def slot(at):
        return o_ref.at[lax.rem(at + 2 * count, count) * 2 + core]

    def ring(step, way, src, at):
        return pltpu.make_async_remote_copy(
            src_ref=src,
            dst_ref=slot(at),
            send_sem=ssem.at[way, step],
            recv_sem=rsem.at[way, step],
            device_id={"ep_0": left if way else right},
            device_id_type=MESH,
        )

    def across(k, src, at):
        return pltpu.make_async_remote_copy(
            src_ref=src,
            dst_ref=slot(at),
            send_sem=dsem.at[k],
            recv_sem=drsem.at[k],
            device_id={"ep_1": twin},
            device_id_type=MESH,
        )

    own = pltpu.make_async_copy(x_ref, slot(z), lsem)
    own.start()
    to_right = [ring(0, 0, x_ref, z)]
    to_left = [ring(0, 1, x_ref, z)]
    to_right[0].start()
    to_left[0].start()
    swaps = [across(0, x_ref, z)]
    swaps[0].start()
    steps_right = count // 2
    steps_left = count - 1 - steps_right
    for step in range(1, steps_right + 1):
        to_right[step - 1].wait_recv()
        if step < steps_right:
            to_right.append(ring(step, 0, slot(z - step), z - step))
            to_right[-1].start()
        swaps.append(across(len(swaps), slot(z - step), z - step))
        swaps[-1].start()
        if step <= steps_left:
            to_left[step - 1].wait_recv()
            if step < steps_left:
                to_left.append(ring(step, 1, slot(z + step), z + step))
                to_left[-1].start()
            swaps.append(across(len(swaps), slot(z + step), z + step))
            swaps[-1].start()
    for copy in to_right + to_left:
        copy.wait_send()
    for copy in swaps:
        copy.wait()
    own.wait()


def gather_keys(block):
    count = lax.axis_size("ep_0")
    half = count // 2
    return pl.pallas_call(
        gather_kernel,
        in_specs=[vspec()],
        out_specs=vspec(),
        out_shape=jax.ShapeDtypeStruct((2 * count, *block.shape), block.dtype),
        scratch_shapes=[
            pltpu.SemaphoreType.DMA((2, half)),
            pltpu.SemaphoreType.DMA((2, half)),
            pltpu.SemaphoreType.DMA((count,)),
            pltpu.SemaphoreType.DMA((count,)),
            pltpu.SemaphoreType.DMA,
        ],
        compiler_params=pltpu.CompilerParams(
            collective_id=0, has_side_effects=True, vmem_limit_bytes=16 * 1024 * 1024
        ),
        cost_estimate=pl.CostEstimate(
            flops=1 << 28, bytes_accessed=64 * block.size, transcendentals=0
        ),
        name="gather_keys",
    )(block)


def attend_kernel(q_ref, kv_ref, o_ref, *, key_block, query_tile):
    head = q_ref.shape[1] // 2
    lane = iota((key_block, 2 * head), 1)
    tiles = q_ref.shape[0] // query_tile

    def step(i, carried):
        block = kv_ref[pl.ds(pl.multiple_of(i * key_block, key_block), key_block), :]
        keys = jnp.concatenate([block[:, :head], block[:, :head]], axis=1)
        values = jnp.where(lane < head, jnp.ones_like(block), block)
        out = []
        for t in range(tiles):
            top, acc = carried[t]
            scores = lax.dot_general(
                q_ref[t * query_tile : (t + 1) * query_tile, :],
                keys,
                (((1,), (1,)), ((), ())),
                preferred_element_type=F32,
            )
            top_new = jnp.maximum(top, jnp.max(scores, axis=1, keepdims=True))
            weights = jnp.exp2(scores - top_new).astype(BF)
            out.append((top_new, acc * jnp.exp2(top - top_new) + mm(weights, values)))
        return tuple(out)

    start = tuple(
        (jnp.full((query_tile, 1), -1e30, F32), jnp.zeros((query_tile, 2 * head), F32))
        for _ in range(tiles)
    )
    ended = lax.fori_loop(0, kv_ref.shape[0] // key_block, step, start)
    for t in range(tiles):
        _, acc = ended[t]
        o_ref[t * query_tile : (t + 1) * query_tile, :] = (acc[:, head:] / acc[:, :1]).astype(BF)


def attend(q_rows, kv, query_tile):
    rows = q_rows.shape[0]
    keys, both = kv.shape
    key_block = next(b for b in (2048, 1024, 512, 256, 128, keys) if keys % b == 0)
    return local_call(
        functools.partial(attend_kernel, key_block=key_block, query_tile=query_tile),
        [jax.ShapeDtypeStruct((rows, both // 2), BF)],
        12 * rows * keys * both,
    )(q_rows, kv)[0]


def moved(x, by):
    count = lax.axis_size("tp")
    return lax.ppermute(x, "tp", [(i, (i + by) % count) for i in range(count)])


def summed(parts):
    total = parts[0].astype(F32)
    for part in parts[1:]:
        total = total + part.astype(F32)
    return total


def body(
    queries,
    key_values,
    query_gain,
    key_gain,
    out_weight,
    second_batch,
    norm_gain,
    routes,
    route_weights,
    expert_gate,
    expert_up,
    expert_down,
    shared_gate,
    shared_up,
    shared_down,
):
    rows = queries.shape[0]
    head = query_gain.shape[0]
    heads = queries.shape[1] // head
    ep_count = lax.axis_size(EP)
    tp_count = lax.axis_size("tp")
    tokens, width = second_batch.shape
    local_experts = expert_gate.shape[0]
    experts = local_experts * ep_count
    piece = width // SPLIT
    chunk_rows = ep_count * CAPACITY * SPLIT
    chunk = jax.ShapeDtypeStruct((chunk_rows, piece), BF)

    normed, *outgoing = local_call(
        functools.partial(prep_kernel, experts=experts, local_experts=local_experts),
        [jax.ShapeDtypeStruct((tokens, width), BF)] + [chunk] * local_experts,
        2 * local_experts * chunk_rows * tokens * width,
    )(second_batch, norm_gain[None, :], routes.T)

    def across(x):
        tiles = x.reshape(ep_count, -1, piece)
        out = lax.all_to_all(tiles, EP, split_axis=0, concat_axis=0, tiled=True)
        return out.reshape(x.shape)

    positions = lax.axis_index(EP) * rows + jnp.arange(rows, dtype=jnp.int32)
    cosine, sine = angle_tables(positions, head)
    q_rows, kv_block = local_call(
        turn_kernel,
        [
            jax.ShapeDtypeStruct((heads * rows, 2 * head), BF),
            jax.ShapeDtypeStruct((rows, 2 * head), BF),
        ],
        1 << 26,
    )(queries, key_values, query_gain[None, :], key_gain[None, :], cosine, sine)
    kv = gather_keys(kv_block)
    kv = kv.reshape(ep_count * rows, 2 * head)

    near = [moved(normed, 1), moved(normed, -1), moved(normed, 2)]
    partial = local_call(
        shared_kernel,
        [jax.ShapeDtypeStruct((tokens, width), BF)] * 4,
        6 * 4 * tokens * width * shared_gate.shape[1],
    )(normed, *near, shared_gate, shared_up, shared_down)
    shared_parts = [partial[0], moved(partial[1], -1), moved(partial[2], 1), moved(partial[3], 2)]

    weights = (expert_gate, expert_up, expert_down)
    returned = []
    half = chunk_rows // 2
    for j in range(local_experts):
        mine = across(outgoing[j])
        from_left = moved(mine, 1)
        from_right = moved(mine, -1)
        far_low = moved(from_left[:half], 1)
        far_high = moved(from_right[half:], -1)
        out = run_experts(
            (mine, from_left, from_right, far_low, far_high),
            ((0,), (1,), (2,), (3, 4)),
            weights,
            j,
        )
        arrived = [out[0], moved(out[1], -1), moved(out[2], 1), moved(out[3], 2)]
        total = summed(arrived).astype(BF)
        returned.append(across(total))

    attended = []
    for h in range(0, heads, 2):
        out = attend(q_rows[h * rows : (h + 2) * rows], kv, rows)
        attended += [out[:rows], out[rows:]]
    head_out = jnp.concatenate(attended, axis=1)
    me = lax.axis_index("tp")
    block = rows // tp_count

    def partial_for(by):
        at = lax.rem(me + by + tp_count, tp_count) * block
        own = lax.dynamic_slice_in_dim(head_out, at, block, 0)
        return jnp.dot(own, out_weight, preferred_element_type=F32).astype(BF)

    mixed = [
        partial_for(0),
        moved(partial_for(1), 1),
        moved(partial_for(-1), -1),
        moved(partial_for(2), 2),
    ]
    attn_sum = summed(mixed).astype(BF)

    combined = local_call(
        functools.partial(combine_kernel, experts=experts, local_experts=local_experts),
        [jax.ShapeDtypeStruct((tokens, width), BF)],
        4 * local_experts * chunk_rows * tokens * width,
    )(*shared_parts, routes, route_weights, *returned)[0]
    return (attn_sum, combined)


def solution(mesh):
    torus = Mesh(
        mesh.devices.reshape(mesh.shape["grp"], mesh.shape["ep"] // 2, 2, mesh.shape["tp"]),
        ("grp", "ep_0", "ep_1", "tp"),
    )

    return jax.shard_map(
        body,
        mesh=torus,
        in_specs=(
            P(GRP_EP, "tp"),
            P(GRP_EP, "tp"),
            P(),
            P(),
            P("tp", None),
            P(GRP_EP_TP, None),
            P(),
            P(GRP_EP_TP, None),
            P(GRP_EP_TP, None),
            P(EP, None, "tp"),
            P(EP, None, "tp"),
            P(EP, "tp", None),
            P(None, "tp"),
            P(None, "tp"),
            P("tp", None),
        ),
        out_specs=(P(GRP_EP_TP, None), P(GRP_EP_TP, None)),
        check_vma=False,
    )
```

```python
import functools

import jax
import jax.numpy as jnp
from jax import lax
from jax.experimental import pallas as pl
from jax.experimental.pallas import tpu as pltpu
from jax.sharding import Mesh
from jax.sharding import PartitionSpec as P

GRID_W = 64
EP = ("ep_0", "ep_1")
GRP_EP = ("grp", "ep_0", "ep_1")
GRP_EP_TP = ("grp", "ep_0", "ep_1", "tp")
MESH = pl.DeviceIdType.MESH
BF = jnp.bfloat16
F32 = jnp.float32
rope_base = 10000.0
norm_eps = 1e-06
LOG2E = 1.4426950408889634
VMEM_BYTES = 60 * 1024 * 1024
CAPACITY = 6
SPLIT = 4


def vspec():
    return pl.BlockSpec(memory_space=pltpu.VMEM)


def local_call(kernel, outs, flops, scratch=(), vmem=VMEM_BYTES):
    def call(*args):
        size = sum(a.size * a.dtype.itemsize for a in (*args, *outs))
        return pl.pallas_call(
            kernel,
            in_specs=[vspec()] * len(args),
            out_specs=[vspec()] * len(outs),
            out_shape=list(outs),
            scratch_shapes=list(scratch),
            compiler_params=pltpu.CompilerParams(vmem_limit_bytes=vmem),
            cost_estimate=pl.CostEstimate(flops=flops, bytes_accessed=size, transcendentals=0),
        )(*args)

    return call


def iota(shape, dim):
    return lax.broadcasted_iota(jnp.int32, shape, dim)


def mm(a, b):
    return jnp.dot(a, b, preferred_element_type=F32)


def slots_in_lanes(routes_t, experts):
    tokens = routes_t.shape[1]
    row = iota((experts, tokens), 0)
    first = (row == routes_t[0:1, :]).astype(F32)
    second = (row == routes_t[1:2, :]).astype(F32)
    before = (iota((tokens, tokens), 0) < iota((tokens, tokens), 1)).astype(BF)
    counts = mm((first + second).astype(BF), before)
    out = []
    for k, hot in enumerate((first, second)):
        within = jnp.sum(counts * hot, axis=0, keepdims=True).astype(jnp.int32)
        out.append(routes_t[k : k + 1, :] * CAPACITY + within)
    return out


def slots_in_rows(routes, experts):
    tokens = routes.shape[0]
    col = iota((tokens, experts), 1)
    first = (col == routes[:, 0:1]).astype(F32)
    second = (col == routes[:, 1:2]).astype(F32)
    before = (iota((tokens, tokens), 1) < iota((tokens, tokens), 0)).astype(BF)
    counts = mm(before, (first + second).astype(BF))
    out = []
    for k, hot in enumerate((first, second)):
        within = jnp.sum(counts * hot, axis=1, keepdims=True).astype(jnp.int32)
        out.append(routes[:, k : k + 1] * CAPACITY + within)
    return out


def slot_of_row(row, local_experts, j):
    per = CAPACITY * SPLIT
    dest = row // per
    quarter = (row % per) // CAPACITY
    place = row % CAPACITY
    return (dest * local_experts + j) * CAPACITY + place, quarter


def prep_kernel(x_ref, gain_ref, routes_t_ref, normed_ref, *chunk_refs, experts, local_experts):
    x = x_ref[...].astype(F32)
    scale = lax.rsqrt(jnp.mean(x * x, axis=-1, keepdims=True) + norm_eps)
    normed_ref[...] = (x * scale * gain_ref[...]).astype(BF)
    tokens, width = x_ref.shape
    piece = width // SPLIT
    slots = slots_in_lanes(routes_t_ref[...], experts)
    for j, out_ref in enumerate(chunk_refs):
        rows = out_ref.shape[0]
        slot, _ = slot_of_row(iota((rows, tokens), 0), local_experts, j)
        hot = ((slot == slots[0]) | (slot == slots[1])).astype(BF)
        _, quarter = slot_of_row(iota((rows, piece), 0), local_experts, j)
        got = jnp.zeros((rows, piece), F32)
        for q in range(SPLIT):
            part = mm(hot, normed_ref[:, q * piece : (q + 1) * piece])
            got = jnp.where(quarter == q, part, got)
        out_ref[...] = got.astype(BF)


def sorter(group):
    per = CAPACITY * SPLIT
    rows = group * per
    to = iota((rows, rows), 0)
    at = iota((rows, rows), 1)
    quarter = to // (group * CAPACITY)
    source = (to % (group * CAPACITY)) // CAPACITY
    place = to % CAPACITY
    return (at == source * per + quarter * CAPACITY + place).astype(BF)


def unsorter(group):
    per = CAPACITY * SPLIT
    rows = group * per
    to = iota((rows, rows), 1)
    at = iota((rows, rows), 0)
    quarter = to // (group * CAPACITY)
    source = (to % (group * CAPACITY)) // CAPACITY
    place = to % CAPACITY
    return (at == source * per + quarter * CAPACITY + place).astype(BF)


def silu(v):
    return v / (1.0 + jnp.exp(-v))


GROUP = 8


def experts_kernel(*refs, parts):
    x_refs = refs[: sum(len(p) for p in parts)]
    gate_ref, up_ref, down_ref = refs[len(x_refs) : len(x_refs) + 3]
    o_refs = refs[len(x_refs) + 3 : len(x_refs) + 3 + len(parts)]
    a_ref, h_ref = refs[len(x_refs) + 3 + len(parts) :]
    per = CAPACITY * SPLIT
    grows = GROUP * per
    places = GROUP * CAPACITY
    piece = x_refs[0].shape[1]
    order = sorter(GROUP)
    back = unsorter(GROUP)
    at = 0
    group = 0
    for p in parts:
        for part in p:
            x_ref = x_refs[at]
            at += 1
            for g in range(x_ref.shape[0] // grows):
                block = mm(order, x_ref[g * grows : (g + 1) * grows, :]).astype(BF)
                for q in range(SPLIT):
                    a_ref[group * places : (group + 1) * places, q * piece : (q + 1) * piece] = block[q * places : (q + 1) * places, :]
                group += 1
    gate = mm(a_ref[...], gate_ref[0])
    up = mm(a_ref[...], up_ref[0])
    h_ref[...] = (silu(gate) * up).astype(BF)
    for q in range(SPLIT):
        a_ref[:, q * piece : (q + 1) * piece] = mm(h_ref[...], down_ref[0, :, q * piece : (q + 1) * piece]).astype(BF)
    per_part = group // len(o_refs)
    for k, o_ref in enumerate(o_refs):
        for g in range(per_part):
            lo = (k * per_part + g) * places
            stacked = jnp.concatenate([a_ref[lo : lo + places, q * piece : (q + 1) * piece] for q in range(SPLIT)], axis=0)
            o_ref[g * grows : (g + 1) * grows, :] = mm(back, stacked).astype(BF)


def run_experts(pieces, parts, weights, j):
    rows, piece = pieces[0].shape
    gate, up, down = weights
    width, hidden = gate.shape[1:]
    outs = [jax.ShapeDtypeStruct((rows, piece), BF)] * len(parts)
    total = rows * len(parts) // SPLIT
    return pl.pallas_call(
        functools.partial(experts_kernel, parts=parts),
        grid=(1,),
        in_specs=[pl.BlockSpec(p.shape, lambda i: (0, 0)) for p in pieces]
        + [
            pl.BlockSpec((1, width, hidden), lambda i: (j, 0, 0)),
            pl.BlockSpec((1, width, hidden), lambda i: (j, 0, 0)),
            pl.BlockSpec((1, hidden, width), lambda i: (j, 0, 0)),
        ],
        out_specs=[pl.BlockSpec((rows, piece), lambda i: (0, 0))] * len(parts),
        out_shape=outs,
        scratch_shapes=[
            pltpu.VMEM((total, width), BF),
            pltpu.VMEM((total, hidden), BF),
        ],
        compiler_params=pltpu.CompilerParams(vmem_limit_bytes=VMEM_BYTES),
        cost_estimate=pl.CostEstimate(
            flops=6 * total * width * hidden,
            bytes_accessed=4 * rows * piece * len(parts) + 6 * width * hidden,
            transcendentals=0,
        ),
    )(*pieces, gate, up, down)


def shared_kernel(*refs):
    x_refs = refs[:4]
    gate_ref, up_ref, down_ref = refs[4:7]
    o_refs = refs[7:]
    for x_ref, o_ref in zip(x_refs, o_refs):
        gate = mm(x_ref[...], gate_ref[...])
        up = mm(x_ref[...], up_ref[...])
        hidden = (silu(gate) * up).astype(BF)
        o_ref[...] = mm(hidden, down_ref[...]).astype(BF)


def combine_kernel(*refs, experts, local_experts, j):
    base_refs = refs[:-4]
    routes_ref, weights_ref, back_ref, o_ref = refs[-4:]
    tokens = routes_ref.shape[0]
    slots = slots_in_rows(routes_ref[...], experts)
    rows, piece = back_ref.shape
    slot, quarter = slot_of_row(iota((tokens, rows), 1), local_experts, j)
    for q in range(SPLIT):
        cols = slice(q * piece, (q + 1) * piece)
        total = base_refs[0][:, cols].astype(F32)
        for ref in base_refs[1:]:
            total = total + ref[:, cols].astype(F32)
        for k in range(2):
            hot = ((slot == slots[k]) & (quarter == q)).astype(BF)
            total = total + weights_ref[:, k : k + 1] * mm(hot, back_ref[...])
        o_ref[:, cols] = total.astype(o_ref.dtype)


def turn_kernel(q_ref, kv_ref, qgain_ref, kgain_ref, cos_ref, sin_ref, q_out_ref, kv_out_ref):
    head = qgain_ref.shape[1]
    heads = q_ref.shape[1] // head
    rows = q_ref.shape[0]
    even = iota((rows, 2 * head), 1) % 2 == 0

    def normed(v, gain):
        return v * lax.rsqrt(jnp.mean(v * v, axis=-1, keepdims=True) + norm_eps) * gain

    def turned(pair):
        after = pltpu.roll(pair, 2 * head - 1, 1)
        before = pltpu.roll(pair, 1, 1)
        other = jnp.where(even, after, before)
        return pair * cos_ref[...] + other * sin_ref[...]

    scale = LOG2E * head**-0.5
    for h in range(0, heads, 2):
        pair = jnp.concatenate(
            [
                normed(q_ref[:, (h + i) * head : (h + i + 1) * head].astype(F32), qgain_ref[...])
                for i in range(2)
            ],
            axis=1,
        )
        both = turned(pair).astype(BF).astype(F32) * scale
        for i in range(2):
            one = both[:, i * head : (i + 1) * head]
            high = one.astype(BF)
            low = (one - high.astype(F32)).astype(BF)
            q_out_ref[(h + i) * rows : (h + i + 1) * rows, :] = jnp.concatenate([high, low], axis=1)
    key = normed(kv_ref[:, :head].astype(F32), kgain_ref[...])
    key = turned(jnp.concatenate([key, key], axis=1)).astype(BF)
    kv_out_ref[...] = jnp.concatenate([key[:, :head], kv_ref[:, head:]], axis=1)


def angle_tables(positions, head):
    half = head // 2
    inverse = rope_base ** (-jnp.arange(0, half, 2, dtype=F32) / half)
    lane = jnp.arange(2 * head, dtype=jnp.int32) % head
    which = lane // 2
    grid_row = (positions // GRID_W).astype(F32)
    grid_column = (positions % GRID_W).astype(F32)
    both = jnp.concatenate([inverse, inverse])[which]
    place = jnp.where(which[None, :] < half // 2, grid_row[:, None], grid_column[:, None])
    angles = place * both[None, :]
    sign = jnp.where(lane % 2 == 0, -1.0, 1.0)
    return jnp.cos(angles), jnp.sin(angles) * sign[None, :]


def gather_kernel(x_ref, o_ref, ssem, rsem, dsem, drsem, lsem):
    z = lax.axis_index("ep_0")
    core = lax.axis_index("ep_1")
    count = lax.axis_size("ep_0")
    right = lax.rem(z + 1, count)
    left = lax.rem(z + count - 1, count)
    twin = 1 - core
    barrier = pltpu.get_barrier_semaphore()
    for peer in ({"ep_0": right}, {"ep_0": left}, {"ep_1": twin}):
        pl.semaphore_signal(barrier, 1, device_id=peer, device_id_type=MESH)
    pl.semaphore_wait(barrier, 3)

    def slot(at):
        return o_ref.at[lax.rem(at + 2 * count, count) * 2 + core]

    def ring(step, way, src, at):
        return pltpu.make_async_remote_copy(
            src_ref=src,
            dst_ref=slot(at),
            send_sem=ssem.at[way, step],
            recv_sem=rsem.at[way, step],
            device_id={"ep_0": left if way else right},
            device_id_type=MESH,
        )

    def across(k, src, at):
        return pltpu.make_async_remote_copy(
            src_ref=src,
            dst_ref=slot(at),
            send_sem=dsem.at[k],
            recv_sem=drsem.at[k],
            device_id={"ep_1": twin},
            device_id_type=MESH,
        )

    own = pltpu.make_async_copy(x_ref, slot(z), lsem)
    own.start()
    to_right = [ring(0, 0, x_ref, z)]
    to_left = [ring(0, 1, x_ref, z)]
    to_right[0].start()
    to_left[0].start()
    swaps = [across(0, x_ref, z)]
    swaps[0].start()
    steps_right = count // 2
    steps_left = count - 1 - steps_right
    for step in range(1, steps_right + 1):
        to_right[step - 1].wait_recv()
        if step < steps_right:
            to_right.append(ring(step, 0, slot(z - step), z - step))
            to_right[-1].start()
        swaps.append(across(len(swaps), slot(z - step), z - step))
        swaps[-1].start()
        if step <= steps_left:
            to_left[step - 1].wait_recv()
            if step < steps_left:
                to_left.append(ring(step, 1, slot(z + step), z + step))
                to_left[-1].start()
            swaps.append(across(len(swaps), slot(z + step), z + step))
            swaps[-1].start()
    for copy in to_right + to_left:
        copy.wait_send()
    for copy in swaps:
        copy.wait()
    own.wait()


def gather_keys(block):
    count = lax.axis_size("ep_0")
    half = count // 2
    return pl.pallas_call(
        gather_kernel,
        in_specs=[vspec()],
        out_specs=vspec(),
        out_shape=jax.ShapeDtypeStruct((2 * count, *block.shape), block.dtype),
        scratch_shapes=[
            pltpu.SemaphoreType.DMA((2, half)),
            pltpu.SemaphoreType.DMA((2, half)),
            pltpu.SemaphoreType.DMA((count,)),
            pltpu.SemaphoreType.DMA((count,)),
            pltpu.SemaphoreType.DMA,
        ],
        compiler_params=pltpu.CompilerParams(
            collective_id=0, has_side_effects=True, vmem_limit_bytes=16 * 1024 * 1024
        ),
        cost_estimate=pl.CostEstimate(
            flops=1 << 28, bytes_accessed=64 * block.size, transcendentals=0
        ),
        name="gather_keys",
    )(block)


def attend_kernel(q_ref, kv_ref, o_ref, *, key_block, query_tile):
    head = q_ref.shape[1] // 2
    lane = iota((key_block, 2 * head), 1)
    tiles = q_ref.shape[0] // query_tile

    def step(i, carried):
        block = kv_ref[pl.ds(pl.multiple_of(i * key_block, key_block), key_block), :]
        keys = jnp.concatenate([block[:, :head], block[:, :head]], axis=1)
        values = jnp.where(lane < head, jnp.ones_like(block), block)
        out = []
        for t in range(tiles):
            top, acc = carried[t]
            scores = lax.dot_general(
                q_ref[t * query_tile : (t + 1) * query_tile, :],
                keys,
                (((1,), (1,)), ((), ())),
                preferred_element_type=F32,
            )
            top_new = jnp.maximum(top, jnp.max(scores, axis=1, keepdims=True))
            weights = jnp.exp2(scores - top_new).astype(BF)
            out.append((top_new, acc * jnp.exp2(top - top_new) + mm(weights, values)))
        return tuple(out)

    start = tuple(
        (jnp.full((query_tile, 1), -1e30, F32), jnp.zeros((query_tile, 2 * head), F32))
        for _ in range(tiles)
    )
    ended = lax.fori_loop(0, kv_ref.shape[0] // key_block, step, start)
    for t in range(tiles):
        _, acc = ended[t]
        o_ref[t * query_tile : (t + 1) * query_tile, :] = (acc[:, head:] / acc[:, :1]).astype(BF)


def attend(q_rows, kv, query_tile):
    rows = q_rows.shape[0]
    keys, both = kv.shape
    key_block = next(b for b in (2048, 1024, 512, 256, 128, keys) if keys % b == 0)
    return local_call(
        functools.partial(attend_kernel, key_block=key_block, query_tile=query_tile),
        [jax.ShapeDtypeStruct((rows, both // 2), BF)],
        12 * rows * keys * both,
    )(q_rows, kv)[0]


def moved(x, by):
    count = lax.axis_size("tp")
    return lax.ppermute(x, "tp", [(i, (i + by) % count) for i in range(count)])


def summed(parts):
    total = parts[0].astype(F32)
    for part in parts[1:]:
        total = total + part.astype(F32)
    return total


def body(
    queries,
    key_values,
    query_gain,
    key_gain,
    out_weight,
    second_batch,
    norm_gain,
    routes,
    route_weights,
    expert_gate,
    expert_up,
    expert_down,
    shared_gate,
    shared_up,
    shared_down,
):
    rows = queries.shape[0]
    head = query_gain.shape[0]
    heads = queries.shape[1] // head
    ep_count = lax.axis_size(EP)
    tp_count = lax.axis_size("tp")
    tokens, width = second_batch.shape
    local_experts = expert_gate.shape[0]
    experts = local_experts * ep_count
    piece = width // SPLIT
    chunk_rows = ep_count * CAPACITY * SPLIT
    chunk = jax.ShapeDtypeStruct((chunk_rows, piece), BF)

    normed, *outgoing = local_call(
        functools.partial(prep_kernel, experts=experts, local_experts=local_experts),
        [jax.ShapeDtypeStruct((tokens, width), BF)] + [chunk] * local_experts,
        2 * local_experts * chunk_rows * tokens * width,
    )(second_batch, norm_gain[None, :], routes.T)

    def across(x):
        tiles = x.reshape(ep_count, -1, piece)
        out = lax.all_to_all(tiles, EP, split_axis=0, concat_axis=0, tiled=True)
        return out.reshape(x.shape)

    positions = lax.axis_index(EP) * rows + jnp.arange(rows, dtype=jnp.int32)
    cosine, sine = angle_tables(positions, head)
    q_rows, kv_block = local_call(
        turn_kernel,
        [
            jax.ShapeDtypeStruct((heads * rows, 2 * head), BF),
            jax.ShapeDtypeStruct((rows, 2 * head), BF),
        ],
        1 << 26,
    )(queries, key_values, query_gain[None, :], key_gain[None, :], cosine, sine)
    kv = gather_keys(kv_block)
    kv = kv.reshape(ep_count * rows, 2 * head)

    near = [moved(normed, 1), moved(normed, -1), moved(normed, 2)]
    partial = local_call(
        shared_kernel,
        [jax.ShapeDtypeStruct((tokens, width), BF)] * 4,
        6 * 4 * tokens * width * shared_gate.shape[1],
    )(normed, *near, shared_gate, shared_up, shared_down)
    shared_parts = [partial[0], moved(partial[1], -1), moved(partial[2], 1), moved(partial[3], 2)]

    weights = (expert_gate, expert_up, expert_down)
    returned = []
    half = chunk_rows // 2
    for j in range(local_experts):
        mine = across(outgoing[j])
        from_left = moved(mine, 1)
        from_right = moved(mine, -1)
        far_low = moved(from_left[:half], 1)
        far_high = moved(from_right[half:], -1)
        out = run_experts(
            (mine, from_left, from_right, far_low, far_high),
            ((0,), (1,), (2,), (3, 4)),
            weights,
            j,
        )
        arrived = [out[0], moved(out[1], -1), moved(out[2], 1), moved(out[3], 2)]
        total = summed(arrived).astype(BF)
        returned.append(across(total))

    attended = []
    for h in range(0, heads, 2):
        out = attend(q_rows[h * rows : (h + 2) * rows], kv, rows)
        attended += [out[:rows], out[rows:]]
    head_out = jnp.concatenate(attended, axis=1)
    me = lax.axis_index("tp")
    block = rows // tp_count

    def partial_for(by):
        at = lax.rem(me + by + tp_count, tp_count) * block
        own = lax.dynamic_slice_in_dim(head_out, at, block, 0)
        return jnp.dot(own, out_weight, preferred_element_type=F32).astype(BF)

    mixed = [
        partial_for(0),
        moved(partial_for(1), 1),
        moved(partial_for(-1), -1),
        moved(partial_for(2), 2),
    ]
    attn_sum = summed(mixed).astype(BF)

    combined = shared_parts
    for j in range(local_experts):
        kept = BF if j == local_experts - 1 else F32
        combined = local_call(
            functools.partial(combine_kernel, experts=experts, local_experts=local_experts, j=j),
            [jax.ShapeDtypeStruct((tokens, width), kept)],
            4 * chunk_rows * tokens * width,
        )(*combined, routes, route_weights, returned[j])
    return (attn_sum, combined[0])


def solution(mesh):
    torus = Mesh(
        mesh.devices.reshape(mesh.shape["grp"], mesh.shape["ep"] // 2, 2, mesh.shape["tp"]),
        ("grp", "ep_0", "ep_1", "tp"),
    )

    return jax.shard_map(
        body,
        mesh=torus,
        in_specs=(
            P(GRP_EP, "tp"),
            P(GRP_EP, "tp"),
            P(),
            P(),
            P("tp", None),
            P(GRP_EP_TP, None),
            P(),
            P(GRP_EP_TP, None),
            P(GRP_EP_TP, None),
            P(EP, None, "tp"),
            P(EP, None, "tp"),
            P(EP, "tp", None),
            P(None, "tp"),
            P(None, "tp"),
            P("tp", None),
        ),
        out_specs=(P(GRP_EP_TP, None), P(GRP_EP_TP, None)),
        check_vma=False,
    )
```
